32 devices in a mesh: grp: 2 (over y), fs: 4 (over z), tp: 4 (over x, core).
Axes of the slice: x: 2, y: 2, z: 4, core: 2. Of those that a mesh axis runs over, the one named last changes fastest.
Arguments:
- inputs: bfloat16 [6144, 2048], P(('grp', 'fs'), 'tp'), parts along dimension 0, may hold values from -110 to 110, as said below
- mixer_gain: float32 [2048], replicated, may hold values from 0.1 to 1.9
- query_weight: bfloat16 [2048, 1024], P('fs', 'tp'), may hold values from -0.125 to 0.125
- key_weight: bfloat16 [2048, 1024], P('fs', 'tp'), may hold values from -0.125 to 0.125
- value_weight: bfloat16 [2048, 1024], P('fs', 'tp'), may hold values from -0.125 to 0.125
- gate_weight: bfloat16 [2048, 1024], P('fs', 'tp'), may hold values from -0.125 to 0.125
- head_gain: float32 [1024], P('tp'), may hold values from 0.1 to 1.9
- out_weight: bfloat16 [1024, 2048], P('tp', 'fs'), may hold values from -0.1875 to 0.1875
- channel_gain: float32 [2048], replicated, may hold values from 0.1 to 1.9
- up_weight: bfloat16 [2048, 5632], P('fs', 'tp'), may hold values from -0.125 to 0.125
- switch_weight: bfloat16 [2048, 5632], P('fs', 'tp'), may hold values from -0.125 to 0.125
- filter_up: float32 [3, 5632], P(None, 'tp'), may hold values from -3.5 to 3.5
- filter_switch: float32 [3, 5632], P(None, 'tp'), may hold values from -3.5 to 3.5
- down_weight: bfloat16 [5632, 2048], P('tp', 'fs'), may hold values from -0.078125 to 0.078125
Outputs:
- layer_output: bfloat16 [6144, 2048], P(('grp', 'fs'), 'tp'), parts along dimension 0
The draws below stay inside these ranges and needn't reach their ends.
There are 2 independent parts, one for each index of `grp`. The reference program is written for one: setup_inputs(seed, part) draws one part's arguments, and reference() takes and returns one part's arrays. A program takes and returns all parts, laid end to end along the dimension named above; an argument that names none is the same for every part. Nothing has to cross between parts.
Inputs may be any that keep to these rules, and one draw needn't show every extreme that they name: `inputs`: activations of one part.
All inputs are finite; a program needn't handle non-finite values.
Results may differ from the reference program's by a relative error of at most 0.012.
Values may be sent and summed in bfloat16 or wider, within the bound.
A program may use at most 64 MiB of HBM per device.

```python
import jax
import jax.numpy as jnp
from jax import lax

D = 2048
HEAD = 128
FF = 5632
KERNEL = 3
TOK_DEV = 768
RET = 1024
TOKENS = 3072
N_FS = 4
N_TP = 4


def draw_inputs(key, part):
    keys_list = jax.random.split(jax.random.fold_in(key, 11), 3)
    trend_line = jnp.log(3.0) * (jnp.arange(D, dtype=jnp.float32) / D - 0.5)
    column_scale = jnp.exp(jax.random.uniform(keys_list[1], (D,), jnp.float32, -1.15, 1.15) + trend_line)
    noise_field = jnp.clip(jax.random.normal(keys_list[0], (TOKENS, D), jnp.float32), -6.0, 6.0)
    row_scale = jnp.exp(jax.random.uniform(keys_list[2], (TOKENS, 1), jnp.float32, -1.15, 1.15))
    return (noise_field * row_scale * column_scale[None, :]).astype(jnp.bfloat16)


def shard_levels(stream_key, shape, cuts, smallest, top_value):
    def one(dim, parts):
        heights = jax.random.uniform(jax.random.fold_in(jax.random.fold_in(stream_key, 6), dim), (parts,), jnp.float32, smallest / len(cuts), top_value / len(cuts))
        return jnp.repeat(jnp.exp(heights), shape[dim] // parts).reshape((-1,) + (1,) * (len(shape) - dim - 1))

    level = one(*cuts[0])
    for cut in cuts[1:]:
        level = level * one(*cut)
    return level


def scatter_about(stream_key, dims, scale, limit, cuts=(), held_as=jnp.bfloat16):
    entries = scale * jax.random.normal(stream_key, dims, jnp.float32)
    if cuts:
        entries = entries * shard_levels(stream_key, dims, cuts, -0.22, 0.18)
    return jnp.clip(entries, -limit, limit).astype(held_as)


def setup_inputs(seed: int = 0, part: int = 0) -> dict:
    keys = jax.random.split(jax.random.key(seed), 15)
    part_splits = jax.random.split(jax.random.fold_in(keys[14], part), 15)
    inputs = draw_inputs(jax.random.fold_in(jax.random.fold_in(keys[14], part), 71), part)
    mixer_gain = jnp.clip(1.0 + 0.18 * jax.random.normal(keys[1], (D,), jnp.float32), 0.1, 1.9)
    query_weight = scatter_about(keys[2], (D, RET), D ** -0.5, 0.125, ((0, 4), (1, 4)))
    key_weight = scatter_about(keys[3], (D, RET), D ** -0.5, 0.125, ((0, 4), (1, 4)))
    value_weight = scatter_about(keys[4], (D, RET), D ** -0.5, 0.125, ((0, 4), (1, 4)))
    gate_weight = scatter_about(keys[5], (D, RET), D ** -0.5, 0.125, ((0, 4), (1, 4)))
    head_gain = jnp.clip(1.0 + 0.18 * jax.random.normal(keys[6], (RET,), jnp.float32), 0.1, 1.9)
    out_weight = scatter_about(keys[7], (RET, D), RET ** -0.5, 0.1875, ((0, 4), (1, 4)))
    channel_gain = jnp.clip(1.0 + 0.18 * jax.random.normal(keys[8], (D,), jnp.float32), 0.1, 1.9)
    up_weight = scatter_about(keys[9], (D, FF), D ** -0.5, 0.125, ((0, 4), (1, 4)))
    switch_weight = scatter_about(keys[10], (D, FF), D ** -0.5, 0.125, ((0, 4), (1, 4)))
    filter_up = scatter_about(keys[11], (KERNEL, FF), KERNEL ** -0.5, 3.5, ((1, 4),), jnp.float32)
    filter_switch = scatter_about(keys[12], (KERNEL, FF), KERNEL ** -0.5, 3.5, ((1, 4),), jnp.float32)
    down_weight = scatter_about(keys[13], (FF, D), FF ** -0.5, 0.078125, ((0, 4), (1, 4)))
    return dict(inputs=inputs, mixer_gain=mixer_gain, query_weight=query_weight, key_weight=key_weight, value_weight=value_weight, gate_weight=gate_weight, head_gain=head_gain, out_weight=out_weight, channel_gain=channel_gain, up_weight=up_weight, switch_weight=switch_weight, filter_up=filter_up, filter_switch=filter_switch, down_weight=down_weight)


epsilon = 1e-06

def row_norm(row_block, gain_vector):
    values = row_block.astype(jnp.float32)
    scaled = values * lax.rsqrt(lax.optimization_barrier(jnp.mean(values * values, axis=-1, keepdims=True)) + epsilon)
    return (scaled * gain_vector.astype(jnp.float32)).astype(jnp.bfloat16)

def rotate(field, positions):
    half_width = field.shape[-1] // 2
    frequency = 10000.0 ** (-jnp.arange(half_width, dtype=jnp.float32) * 2.0 / field.shape[-1])
    angles = positions.astype(jnp.float32)[:, None] * frequency[None, :]
    cosine = jnp.cos(angles)[:, None, :]
    sine_part = jnp.sin(angles)[:, None, :]
    first_half = field[..., :half_width]
    second_half = field[..., half_width:]
    return jnp.concatenate([first_half * cosine - second_half * sine_part, first_half * sine_part + second_half * cosine], axis=-1)

def decays(first_head, count, positions):
    head_ids = (first_head + jnp.arange(count, dtype=jnp.int32)).astype(jnp.float32)
    log_decay = jnp.log1p(-jnp.exp2(-5.0 - head_ids))
    causal = positions[:, None] >= positions[None, :]
    distance = jnp.where(causal, positions[:, None] - positions[None, :], 0).astype(jnp.float32)
    return jnp.where(causal[None], jnp.exp(log_decay[:, None, None] * distance[None]), 0.0)

def retention(query_rows, key_rows, value_rows, gate_rows, gain_vector):
    length = query_rows.shape[0]
    count = query_rows.shape[1] // HEAD
    positions = jnp.arange(length, dtype=jnp.int32)
    query_rot = rotate(query_rows.astype(jnp.float32).reshape(length, count, HEAD), positions).astype(jnp.bfloat16)
    key_rot = rotate(key_rows.astype(jnp.float32).reshape(length, count, HEAD), positions).astype(jnp.bfloat16)
    decay_table = decays(0, count, positions)
    scores = jnp.einsum('thd,shd->hts', query_rot.astype(jnp.float32), key_rot.astype(jnp.float32))
    weights = (scores * HEAD ** (-0.5) * decay_table).astype(jnp.bfloat16)
    values = value_rows.reshape(length, count, HEAD).astype(jnp.float32)
    retained = jnp.einsum('hts,shd->thd', weights.astype(jnp.float32), values)
    normalized = retained * lax.rsqrt(lax.optimization_barrier(jnp.mean(retained * retained, axis=-1, keepdims=True)) + epsilon)
    gated_rows = normalized.reshape(length, count * HEAD) * gain_vector * jax.nn.silu(gate_rows.astype(jnp.float32))
    return gated_rows.astype(jnp.bfloat16)

def causal_conv(row_block, tap_weights, length):
    sequences = row_block.astype(jnp.float32).reshape(-1, length, row_block.shape[1])
    width_taps = tap_weights.shape[0]
    padded = jnp.pad(sequences, ((0, 0), (width_taps - 1, 0), (0, 0)))
    result = jnp.zeros_like(sequences)
    for tap_index in range(width_taps):
        result = result + padded[:, tap_index:tap_index + length] * tap_weights[tap_index].astype(jnp.float32)
    return result.reshape(row_block.shape)

def grouped_sum(left_side, right_side, groups):
    block_width = left_side.shape[1] // groups
    result = jnp.zeros((left_side.shape[0], right_side.shape[1]), jnp.float32)
    for group_index in range(groups):
        lower = group_index * block_width
        part_sum = jnp.dot(left_side[:, lower:lower + block_width], right_side[lower:lower + block_width], preferred_element_type=jnp.float32)
        result = result + lax.optimization_barrier(part_sum.astype(jnp.bfloat16)).astype(jnp.float32)
    return result

def reference(inputs, mixer_gain, query_weight, key_weight, value_weight, gate_weight, head_gain, out_weight, channel_gain, up_weight, switch_weight, filter_up, filter_switch, down_weight):
    normed = row_norm(inputs, mixer_gain)
    projected = [jnp.dot(normed, matrix, preferred_element_type=jnp.float32).astype(jnp.bfloat16) for matrix in (query_weight, key_weight, value_weight, gate_weight)]
    shaped = tuple((block.reshape(N_FS, TOK_DEV, block.shape[1]) for block in projected))

    def one_sequence(pieces):
        return retention(pieces[0], pieces[1], pieces[2], pieces[3], head_gain)
    head_out = lax.map(one_sequence, shaped).reshape(inputs.shape[0], -1)
    mixer_sum = grouped_sum(head_out, out_weight, N_TP)
    mixed_rows = (inputs.astype(jnp.float32) + mixer_sum).astype(jnp.bfloat16)
    channel_normed = row_norm(mixed_rows, channel_gain)
    lifted = jnp.dot(channel_normed, up_weight, preferred_element_type=jnp.float32).astype(jnp.bfloat16)
    switched = jnp.dot(channel_normed, switch_weight, preferred_element_type=jnp.float32).astype(jnp.bfloat16)
    lift_mixed = causal_conv(lifted, filter_up, TOK_DEV)
    switch_mixed = causal_conv(switched, filter_switch, TOK_DEV)
    hidden = (lift_mixed * jax.nn.silu(switch_mixed)).astype(jnp.bfloat16)
    channel_sum = grouped_sum(hidden, down_weight, N_TP)
    return (mixed_rows.astype(jnp.float32) + channel_sum).astype(jnp.bfloat16)
```

```python
import functools

import jax
import jax.numpy as jnp
from jax import lax
from jax.experimental import pallas as pl
from jax.experimental.pallas import tpu as pltpu
from jax.sharding import PartitionSpec as P

HEAD = 128
EPS = 1e-06
MESH = pl.DeviceIdType.MESH
BF = jnp.bfloat16
F32 = jnp.float32


def chunks_of(rows):
    return 2 if rows % 32 == 0 else 1


def kernel(cfg, x_hbm, mg, q_hbm, k_hbm, v_hbm, g_hbm, hg, ow_hbm, cg, up_hbm, sw_hbm, fu, fsw, dn_hbm,
           cos_ref, sin_ref, ld_ref, o_ref,
           wq, ob, ub, sb, db, xw, xn, qr, kr, vr, gr, ho, part, ra, st, rb, mw, lift, swit, hid,
           part2, ra2, st2, rb2,
           loc, zs, zr, ys, yr, a1s, a1r, a2s, a2r, b1s, b1r, b2s, b2r, c1s, c1r, c2s, c2r, d1s, d1r, d2s, d2r):
    n_g, n_f, n_t = cfg
    n_x = n_t // 2
    grp, z, t = lax.axis_index("grp"), lax.axis_index("fs"), lax.axis_index("tp")
    x, c = t // 2, t % 2
    partner = x * 2 + (1 - c)
    T, bw = x_hbm.shape
    D = bw * n_t
    RC = 256
    R = T // RC
    width = q_hbm.shape[1]
    heads = width // HEAD
    F = up_hbm.shape[1]
    fr = q_hbm.shape[0]
    slotw = ow_hbm.shape[1]
    per_block = bw // slotw

    def rows_of(r, size=RC):
        return pl.ds(r * size if isinstance(r, int) else pl.multiple_of(r * size, size), size)

    barrier = pltpu.get_barrier_semaphore()
    friends = [(grp, lax.rem(z + 1, n_f), t), (grp, lax.rem(z + n_f - 1, n_f), t), (grp, z, partner)]
    friends += [(lax.rem(grp + d, n_g), z, t) for d in range(1, n_g)]
    friends += [(grp, z, lax.rem(x + d, n_x) * 2 + c) for d in range(1, n_x)]
    for f in friends:
        pl.semaphore_signal(barrier, inc=1, device_id=f, device_id_type=MESH)

    zrow = pl.multiple_of(z * fr, fr)
    local = [pltpu.make_async_copy(x_hbm, xw.at[t], loc.at[0])]
    for i, w in enumerate((q_hbm, k_hbm, v_hbm, g_hbm)):
        local.append(pltpu.make_async_copy(
            w, wq.at[pl.ds(zrow, fr), pl.ds(i * width, width)], loc.at[1 + i]))
    local.append(pltpu.make_async_copy(ow_hbm, ob.at[z], loc.at[5]))
    local.append(pltpu.make_async_copy(up_hbm, ub.at[pl.ds(zrow, fr), :], loc.at[6]))
    local.append(pltpu.make_async_copy(sw_hbm, sb.at[pl.ds(zrow, fr), :], loc.at[7]))
    local.append(pltpu.make_async_copy(dn_hbm, db.at[z], loc.at[8]))
    for cp in local:
        cp.start()

    pending = []

    pieces = []

    def add_pieces(buf, slotted, shard, name):
        half = shard // n_g
        count = 1 if name == "out" else chunks_of(half)
        size = half // count
        for j in range(count):
            def ref(src, owner, j=j):
                if slotted:
                    lo = owner * half + j * size
                    return buf.at[src, pl.ds(pl.multiple_of(lo, size), size), :]
                lo = src * shard + owner * half + j * size
                return buf.at[pl.ds(pl.multiple_of(lo, size), size), :]
            pieces.append((name, ref))

    add_pieces(wq, False, fr, "qkvg")
    add_pieces(ob, True, ow_hbm.shape[0], "out")
    add_pieces(ub, False, fr, "up")
    add_pieces(sb, False, fr, "switch")
    add_pieces(db, True, dn_hbm.shape[0], "down")
    n_p = len(pieces)

    def z_copy(p, src, step, way):
        ref = pieces[p][1](src, grp)
        return pltpu.make_async_remote_copy(
            src_ref=ref, dst_ref=ref, send_sem=zs.at[p, 2 * step + way], recv_sem=zr.at[p, src],
            device_id=(grp, z + (1 if way == 0 else -1), t), device_id_type=MESH)

    def y_copy(p, src, d):
        ref = pieces[p][1](src, grp)
        return pltpu.make_async_remote_copy(
            src_ref=ref, dst_ref=ref, send_sem=ys.at[p, src * n_g + d], recv_sem=yr.at[p, src * n_g + grp],
            device_id=(lax.rem(grp + d, n_g), z, t), device_id_type=MESH)

    def z_send(p, src, step, way, cond):
        cp = z_copy(p, src, step, way)

        @pl.when(cond)
        def _():
            cp.start()

        pending.append((cond, cp))

    def own(p):
        z_send(p, z, 0, 0, z < n_f - 1)
        z_send(p, z, 0, 1, z > 0)

    def event(p, s):
        for way in (0, 1):
            src = z - s if way == 0 else z + s
            here = (src >= 0) if way == 0 else (src < n_f)
            safe = jnp.clip(src, 0, n_f - 1)

            @pl.when(here)
            def _():
                z_copy(p, safe, s, way).wait_recv()

            onward = jnp.logical_and(here, z < n_f - 1 if way == 0 else z > 0)
            z_send(p, safe, s, way, onward)
            for d in range(1, n_g):
                cp = y_copy(p, safe, d)

                @pl.when(here)
                def _():
                    cp.start()

                pending.append((here, cp))

    def arrive(p):
        for s in range(1, n_f):
            src = lax.rem(z + s, n_f)
            for d in range(1, n_g):
                owner = lax.rem(grp + d, n_g)
                ref = pieces[p][1](src, owner)
                pltpu.make_async_remote_copy(
                    src_ref=ref, dst_ref=ref, send_sem=ys.at[p, src * n_g],
                    recv_sem=yr.at[p, src * n_g + owner],
                    device_id=(owner, z, t), device_id_type=MESH).wait_recv()

    state = {"own": 0, "ev": 0}
    order = [(p, s) for p in range(n_p) for s in range(1, n_f)]

    def send_own(upto):
        while state["own"] < min(upto, n_p):
            own(state["own"])
            state["own"] += 1

    def pump(count=1):
        for _ in range(count):
            if state["ev"] < len(order):
                p, s = order[state["ev"]]
                send_own(p + 2)
                event(p, s)
                state["ev"] += 1

    def pump_through(name):
        last = max(i for i, pc in enumerate(pieces) if pc[0] == name)
        while state["ev"] < len(order) and order[state["ev"]][0] <= last:
            pump()

    def arrive_all(name):
        pump_through(name)
        for i, pc in enumerate(pieces):
            if pc[0] == name:
                arrive(i)

    def ag_copy(buf, src_x, r, dest, ssem, rsem):
        ref = buf.at[src_x * 2 + c, rows_of(r), :]
        return pltpu.make_async_remote_copy(
            src_ref=ref, dst_ref=ref, send_sem=ssem, recv_sem=rsem,
            device_id=(grp, z, dest), device_id_type=MESH)

    def go(cp):
        cp.start()
        pending.append((None, cp))

    def ag_start(buf, r, sems):
        s1, r1, s2, r2 = sems
        for d in range(1, n_x):
            go(ag_copy(buf, x, r, lax.rem(x + d, n_x) * 2 + c, s1.at[d, r], r1.at[x, r]))
        go(ag_copy(buf, x, r, partner, s2.at[x, r], r2.at[x, r]))

    def ag_forward(buf, r, sems):
        s1, r1, s2, r2 = sems
        for d in range(1, n_x):
            sx = lax.rem(x + d, n_x)
            ag_copy(buf, sx, r, partner, s1.at[d, r], r1.at[sx, r]).wait_recv()
            go(ag_copy(buf, sx, r, partner, s2.at[sx, r], r2.at[sx, r]))

    def ag_finish(buf, r, sems):
        s1, r1, s2, r2 = sems
        for sx in range(n_x):
            ref = buf.at[sx * 2 + (1 - c), rows_of(r), :]
            pltpu.make_async_remote_copy(
                src_ref=ref, dst_ref=ref, send_sem=s2.at[sx, r], recv_sem=r2.at[sx, r],
                device_id=(grp, z, partner), device_id_type=MESH).wait_recv()

    def norm_rows(src, gain, r):
        def body(i, _):
            rows = rows_of(r * (RC // 64) + i, 64)
            total = jnp.zeros((64, 1), F32)
            for b in range(n_t):
                val = src[b, rows, :].astype(F32)
                total = total + jnp.sum(val * val, axis=-1, keepdims=True)
            inv = lax.rsqrt(total / D + EPS)
            for b in range(n_t):
                val = src[b, rows, :].astype(F32)
                xn[rows, b * bw:(b + 1) * bw] = (val * inv * gain[:, b * bw:(b + 1) * bw]).astype(BF)
            return 0
        lax.fori_loop(0, RC // 64, body, 0)

    def product(lhs, rhs, dst, block, r):
        for j in range(per_block):
            dst[block, rows_of(r), j * slotw:(j + 1) * slotw] = jnp.dot(
                lhs[rows_of(r), :], rhs[block * per_block + j], preferred_element_type=F32).astype(BF)

    def rs_copy(src_ref, dst_ref, dest, ssem, rsem):
        return pltpu.make_async_remote_copy(
            src_ref=src_ref, dst_ref=dst_ref, send_sem=ssem, recv_sem=rsem,
            device_id=(grp, z, dest), device_id_type=MESH)

    def reduce(lhs, rhs, prt, r_a, stage, r_b, sems, base, emit, between):
        s1, r1, s2, r2 = sems

        def to_partner(d, r):
            bx = lax.rem(x + d, n_x)
            return rs_copy(prt.at[bx * 2 + 1 - c, rows_of(r), :], r_a.at[d, rows_of(r), :],
                           partner, s1.at[d, r], r1.at[d, r])

        def across(d, r):
            return rs_copy(stage.at[d, rows_of(r), :], r_b.at[d, rows_of(r), :],
                           lax.rem(x + d, n_x) * 2 + c, s2.at[d, r], r2.at[d, r])

        def combine(d, r):
            bx = lax.rem(x + d, n_x)
            to_partner(d, r).wait_recv()
            stage[d, rows_of(r), :] = (prt[bx * 2 + c, rows_of(r), :].astype(F32)
                                       + r_a[d, rows_of(r), :].astype(F32)).astype(BF)
            go(across(d, r))

        work = [(d, r) for d in range(1, n_x) for r in range(R)]
        prev = None
        for d, r in work + [(0, r) for r in range(R)]:
            bx = lax.rem(x + d, n_x)
            product(lhs, rhs, prt, bx * 2 + 1 - c, r)
            go(to_partner(d, r))
            product(lhs, rhs, prt, bx * 2 + c, r)
            if prev is not None and prev[0] > 0:
                combine(*prev)
            prev = (d, r)
            between()
        for r in range(R):
            to_partner(0, r).wait_recv()
            total = prt[t, rows_of(r), :].astype(F32) + r_a[0, rows_of(r), :].astype(F32)
            for d in range(1, n_x):
                across(d, r).wait_recv()
                total = total + r_b[d, rows_of(r), :].astype(F32)
            emit(r, (base[t, rows_of(r), :].astype(F32) + total).astype(BF))

    pl.semaphore_wait(barrier, len(friends))
    local[0].wait()
    agx = (a1s, a1r, a2s, a2r)
    for r in range(R):
        ag_start(xw, r, agx)
    for cp in local[1:]:
        cp.wait()
    send_own(2)
    pump(1)
    for r in range(R):
        ag_forward(xw, r, agx)
    pump(1)
    for r in range(R):
        ag_finish(xw, r, agx)
        norm_rows(xw, mg, r)
        pump(1)
    arrive_all("qkvg")
    send_own(5)

    def project(r, _):
        rows = rows_of(r)
        lhs = xn[rows, :]
        for i, dst in enumerate((qr, kr, vr, gr)):
            val = jnp.dot(lhs, wq[:, i * width:(i + 1) * width], preferred_element_type=F32).astype(BF)
            if i >= 2:
                dst[rows, :] = val
                continue
            for h in range(heads):
                part_h = val[:, h * HEAD:(h + 1) * HEAD].astype(F32)
                dst[rows, h * HEAD:(h + 1) * HEAD] = (
                    part_h * cos_ref[rows, :] + pltpu.roll(part_h, HEAD // 2, 1) * sin_ref[rows, :]).astype(BF)
        return 0

    lax.fori_loop(0, R, project, 0)
    pump(2)
    for h in range(heads):
        cols = slice(h * HEAD, (h + 1) * HEAD)
        for r in range(R):
            span = (r + 1) * RC
            qh = qr[r * RC:(r + 1) * RC, cols]
            scores = lax.dot_general(qh, kr[0:span, cols], (((1,), (1,)), ((), ())),
                                     preferred_element_type=F32)
            gap = (r * RC + lax.broadcasted_iota(jnp.int32, (RC, span), 0)
                   - lax.broadcasted_iota(jnp.int32, (RC, span), 1))
            causal = gap >= 0
            rate = ld_ref[h:h + 1, 0:1]
            fade = jnp.where(causal, jnp.exp(rate * jnp.where(causal, gap, 0).astype(F32)), 0.0)
            weights = (scores * HEAD ** (-0.5) * fade).astype(BF)
            kept = jnp.dot(weights, vr[0:span, cols], preferred_element_type=F32)
            kept = kept * lax.rsqrt(jnp.mean(kept * kept, axis=-1, keepdims=True) + EPS)
            gate = gr[r * RC:(r + 1) * RC, cols].astype(F32)
            ho[r * RC:(r + 1) * RC, cols] = (kept * hg[:, cols] * (gate / (1.0 + jnp.exp(-gate)))).astype(BF)
    arrive_all("out")
    send_own(6)
    agm = (c1s, c1r, c2s, c2r)

    def emit_mixed(r, val):
        mw[t, rows_of(r), :] = val
        ag_start(mw, r, agm)

    reduce(ho, ob, part, ra, st, rb, (b1s, b1r, b2s, b2r), xw, emit_mixed, lambda: None)
    pump(1)
    for r in range(R):
        ag_forward(mw, r, agm)
    pump(1)
    for r in range(R):
        ag_finish(mw, r, agm)
        norm_rows(mw, cg, r)
    arrive_all("up")

    lift[0:16, :] = jnp.zeros((16, F), BF)
    swit[0:16, :] = jnp.zeros((16, F), BF)

    def widen(weights, dst, r):
        dst[pl.ds(16 + r * RC, RC), :] = jnp.dot(
            xn[rows_of(r), :], weights[...], preferred_element_type=F32).astype(BF)

    for r in range(R):
        widen(ub, lift, r)
        pump(1)
    arrive_all("switch")
    edges = list(range(0, F, 256)) + [F]

    def conv_rows(i, _):
        for lo, hi in zip(edges[:-1], edges[1:]):
            mixed = []
            for src, taps in ((lift, fu), (swit, fsw)):
                val = src[pl.ds(pl.multiple_of(i * 64, 64), 80), lo:hi].astype(F32)
                acc = pltpu.roll(val, 2, 0)[16:] * taps[0:1, lo:hi]
                acc = acc + pltpu.roll(val, 1, 0)[16:] * taps[1:2, lo:hi]
                mixed.append(acc + val[16:] * taps[2:3, lo:hi])
            a, b = mixed
            hid[rows_of(i, 64), lo:hi] = (a * (b / (1.0 + jnp.exp(-b)))).astype(BF)
        return 0

    for r in range(R):
        widen(sb, swit, r)
        lax.fori_loop(r * (RC // 64), (r + 1) * (RC // 64), conv_rows, 0)
        pump(1)
    arrive_all("down")

    def emit_out(r, val):
        o_ref[rows_of(r), :] = val

    reduce(hid, db, part2, ra2, st2, rb2, (d1s, d1r, d2s, d2r), mw, emit_out, lambda: None)

    for cond, cp in pending:
        if cond is None:
            cp.wait_send()
        else:
            @pl.when(cond)
            def _(cp=cp):
                cp.wait_send()


def on_device(cfg, inputs, mixer_gain, query_weight, key_weight, value_weight, gate_weight, head_gain,
              out_weight, channel_gain, up_weight, switch_weight, filter_up, filter_switch, down_weight):
    n_g, n_f, n_t = cfg
    n_x = n_t // 2
    T, bw = inputs.shape
    D = bw * n_t
    fr, width = query_weight.shape
    heads = width // HEAD
    F = up_weight.shape[1]
    slotw = out_weight.shape[1]
    half = HEAD // 2
    frequency = 10000.0 ** (-jnp.arange(half, dtype=F32) * 2.0 / HEAD)
    angles = jnp.arange(T, dtype=jnp.int32).astype(F32)[:, None] * frequency[None, :]
    cosine, sine = jnp.cos(angles), jnp.sin(angles)
    cos2 = jnp.concatenate([cosine, cosine], axis=1)
    sin2 = jnp.concatenate([-sine, sine], axis=1)
    ids = (lax.axis_index("tp") * heads + jnp.arange(heads, dtype=jnp.int32)).astype(F32)
    rate = jnp.broadcast_to(jnp.log1p(-jnp.exp2(-5.0 - ids))[:, None], (heads, 128))

    n_p = (chunks_of(fr // n_g) * 3 + 1 + chunks_of(down_weight.shape[0] // n_g))
    R = T // 256
    dma = pltpu.SemaphoreType.DMA
    anyspec = pl.BlockSpec(memory_space=pl.ANY)
    vspec = pl.BlockSpec(memory_space=pltpu.VMEM)
    tp_sems = [dma((n_x, R))] * 16
    act = pltpu.VMEM((n_t, T, bw), BF)
    xblk = pltpu.VMEM((n_x, T, bw), BF)
    scratch = [
        pltpu.VMEM((D, 4 * width), BF),
        pltpu.VMEM((n_f,) + out_weight.shape, BF),
        pltpu.VMEM((D, F), BF),
        pltpu.VMEM((D, F), BF),
        pltpu.VMEM((n_f,) + down_weight.shape, BF),
        act,
        pltpu.VMEM((T, D), BF),
        pltpu.VMEM((T, width), BF), pltpu.VMEM((T, width), BF),
        pltpu.VMEM((T, width), BF), pltpu.VMEM((T, width), BF),
        pltpu.VMEM((T, width), BF),
        act, xblk, xblk, xblk,
        act,
        pltpu.VMEM((T + 16, F), BF), pltpu.VMEM((T + 16, F), BF), pltpu.VMEM((T, F), BF),
        act, xblk, xblk, xblk,
        dma((9,)),
        dma((n_p, 2 * n_f)), dma((n_p, n_f)), dma((n_p, n_f * n_g)), dma((n_p, n_f * n_g)),
    ] + tp_sems
    flops = 2 * T * (D * 4 * width + width * D + 3 * D * F)
    call = pl.pallas_call(
        functools.partial(kernel, cfg),
        out_shape=jax.ShapeDtypeStruct((T, bw), BF),
        in_specs=[anyspec, vspec, anyspec, anyspec, anyspec, anyspec, vspec, anyspec, vspec, anyspec, anyspec,
                  vspec, vspec, anyspec, vspec, vspec, vspec],
        out_specs=vspec,
        scratch_shapes=scratch,
        compiler_params=pltpu.CompilerParams(
            collective_id=0, has_side_effects=True, vmem_limit_bytes=67043328),
        cost_estimate=pl.CostEstimate(flops=flops, bytes_accessed=2 * (D * F * 3), transcendentals=0),
    )
    return call(inputs, mixer_gain[None, :], query_weight, key_weight, value_weight, gate_weight,
                head_gain[None, :], out_weight, channel_gain[None, :], up_weight, switch_weight,
                filter_up, filter_switch, down_weight, cos2, sin2, rate)


def solution(mesh):
    cfg = (mesh.shape["grp"], mesh.shape["fs"], mesh.shape["tp"])
    return jax.shard_map(
        functools.partial(on_device, cfg),
        mesh=mesh,
        in_specs=(
            P(("grp", "fs"), "tp"),
            P(),
            P("fs", "tp"),
            P("fs", "tp"),
            P("fs", "tp"),
            P("fs", "tp"),
            P("tp"),
            P("tp", "fs"),
            P(),
            P("fs", "tp"),
            P("fs", "tp"),
            P(None, "tp"),
            P(None, "tp"),
            P("tp", "fs"),
        ),
        out_specs=P(("grp", "fs"), "tp"),
        check_vma=False,
    )
```

```python
import functools

import jax
import jax.numpy as jnp
from jax import lax
from jax.experimental import pallas as pl
from jax.experimental.pallas import tpu as pltpu
from jax.sharding import PartitionSpec as P

HEAD = 128
EPS = 1e-06
MESH = pl.DeviceIdType.MESH
BF = jnp.bfloat16
F32 = jnp.float32


def chunks_of(rows, most=2):
    while rows % (16 * most):
        most //= 2
    return most


def kernel(cfg, x_hbm, mg, q_hbm, k_hbm, v_hbm, g_hbm, hg, ow_hbm, cg, up_hbm, sw_hbm, fu, fsw, dn_hbm,
           cos_ref, sin_ref, ld_ref, o_ref,
           wq, ob, ub, sb, db, xw, xn, qr, kr, vr, gr, ho, part, ra, st, rb, mw, lift, swit, hid,
           part2, ra2, st2, rb2,
           loc, zs, zr, ys, yr, a1s, a1r, a2s, a2r, b1s, b1r, b2s, b2r, c1s, c1r, c2s, c2r, d1s, d1r, d2s, d2r):
    n_g, n_f, n_t = cfg
    n_x = n_t // 2
    grp, z, t = lax.axis_index("grp"), lax.axis_index("fs"), lax.axis_index("tp")
    x, c = t // 2, t % 2
    partner = x * 2 + (1 - c)
    T, bw = x_hbm.shape
    D = bw * n_t
    RC = 256
    R = T // RC
    width = q_hbm.shape[1]
    heads = width // HEAD
    F = up_hbm.shape[1]
    fr = q_hbm.shape[0]
    slotw = ow_hbm.shape[1]
    per_block = bw // slotw

    def rows_of(r, size=RC):
        return pl.ds(r * size if isinstance(r, int) else pl.multiple_of(r * size, size), size)

    barrier = pltpu.get_barrier_semaphore()
    friends = [(grp, lax.rem(z + 1, n_f), t), (grp, lax.rem(z + n_f - 1, n_f), t), (grp, z, partner)]
    friends += [(lax.rem(grp + d, n_g), z, t) for d in range(1, n_g)]
    friends += [(grp, z, lax.rem(x + d, n_x) * 2 + c) for d in range(1, n_x)]
    for f in friends:
        pl.semaphore_signal(barrier, inc=1, device_id=f, device_id_type=MESH)

    zrow = pl.multiple_of(z * fr, fr)
    local = [pltpu.make_async_copy(x_hbm, xw.at[t], loc.at[0])]
    for i, w in enumerate((q_hbm, k_hbm, v_hbm, g_hbm)):
        local.append(pltpu.make_async_copy(
            w, wq.at[pl.ds(zrow, fr), pl.ds(i * width, width)], loc.at[1 + i]))
    local.append(pltpu.make_async_copy(ow_hbm, ob.at[z], loc.at[5]))
    local.append(pltpu.make_async_copy(up_hbm, ub.at[pl.ds(zrow, fr), :], loc.at[6]))
    local.append(pltpu.make_async_copy(sw_hbm, sb.at[pl.ds(zrow, fr), :], loc.at[7]))
    local.append(pltpu.make_async_copy(dn_hbm, db.at[z], loc.at[8]))
    for cp in local:
        cp.start()

    pending = []

    pieces = []

    def add_pieces(buf, slotted, shard, name):
        half = shard // n_g
        count = 1 if name == "out" else chunks_of(half, 4 if name == "down" else 2)
        size = half // count
        for j in range(count):
            def ref(src, owner, j=j):
                if slotted:
                    lo = owner * half + j * size
                    return buf.at[src, pl.ds(pl.multiple_of(lo, size), size), :]
                lo = src * shard + owner * half + j * size
                return buf.at[pl.ds(pl.multiple_of(lo, size), size), :]
            pieces.append((name, ref))

    add_pieces(wq, False, fr, "qkvg")
    add_pieces(ob, True, ow_hbm.shape[0], "out")
    add_pieces(ub, False, fr, "up")
    add_pieces(sb, False, fr, "switch")
    add_pieces(db, True, dn_hbm.shape[0], "down")
    n_p = len(pieces)

    def z_copy(p, src, step, way):
        ref = pieces[p][1](src, grp)
        return pltpu.make_async_remote_copy(
            src_ref=ref, dst_ref=ref, send_sem=zs.at[p, 2 * step + way], recv_sem=zr.at[p, src],
            device_id=(grp, z + (1 if way == 0 else -1), t), device_id_type=MESH)

    def y_copy(p, src, d):
        ref = pieces[p][1](src, grp)
        return pltpu.make_async_remote_copy(
            src_ref=ref, dst_ref=ref, send_sem=ys.at[p, src * n_g + d], recv_sem=yr.at[p, src * n_g + grp],
            device_id=(lax.rem(grp + d, n_g), z, t), device_id_type=MESH)

    def z_send(p, src, step, way, cond):
        cp = z_copy(p, src, step, way)

        @pl.when(cond)
        def _():
            cp.start()

        pending.append((cond, cp))

    def own(p):
        z_send(p, z, 0, 0, z < n_f - 1)
        z_send(p, z, 0, 1, z > 0)

    def event(p, s):
        for way in (0, 1):
            src = z - s if way == 0 else z + s
            here = (src >= 0) if way == 0 else (src < n_f)
            safe = jnp.clip(src, 0, n_f - 1)

            @pl.when(here)
            def _():
                z_copy(p, safe, s, way).wait_recv()

            onward = jnp.logical_and(here, z < n_f - 1 if way == 0 else z > 0)
            z_send(p, safe, s, way, onward)
            for d in range(1, n_g):
                cp = y_copy(p, safe, d)

                @pl.when(here)
                def _():
                    cp.start()

                pending.append((here, cp))

    def arrive_from(p, src):
        for d in range(1, n_g):
            owner = lax.rem(grp + d, n_g)
            ref = pieces[p][1](src, owner)
            pltpu.make_async_remote_copy(
                src_ref=ref, dst_ref=ref, send_sem=ys.at[p, src * n_g],
                recv_sem=yr.at[p, src * n_g + owner],
                device_id=(owner, z, t), device_id_type=MESH).wait_recv()

    def arrive(p):
        for s in range(1, n_f):
            arrive_from(p, lax.rem(z + s, n_f))

    state = {"own": 0, "ev": 0}
    downs = [i for i, pc in enumerate(pieces) if pc[0] == "down"]
    by_source = per_block == 1
    order = [(p, s) for p in range(n_p) for s in range(1, n_f) if not (by_source and p in downs)]
    if by_source:
        order += [(p, s) for s in range(1, n_f) for p in downs]

    def send_own(upto):
        while state["own"] < min(upto, n_p):
            own(state["own"])
            state["own"] += 1

    def pump(count=1):
        for _ in range(count):
            if state["ev"] < len(order):
                p, s = order[state["ev"]]
                send_own(p + 3)
                event(p, s)
                state["ev"] += 1

    def pump_through(name):
        last = max(i for i, pc in enumerate(pieces) if pc[0] == name)
        while state["ev"] < len(order) and order[state["ev"]][0] <= last:
            pump()

    def arrive_all(name):
        pump_through(name)
        for i, pc in enumerate(pieces):
            if pc[0] == name:
                arrive(i)

    def ag_copy(buf, src_x, r, dest, ssem, rsem):
        ref = buf.at[src_x * 2 + c, rows_of(r), :]
        return pltpu.make_async_remote_copy(
            src_ref=ref, dst_ref=ref, send_sem=ssem, recv_sem=rsem,
            device_id=(grp, z, dest), device_id_type=MESH)

    def go(cp):
        cp.start()
        pending.append((None, cp))

    def ag_start(buf, r, sems):
        s1, r1, s2, r2 = sems
        for d in range(1, n_x):
            go(ag_copy(buf, x, r, lax.rem(x + d, n_x) * 2 + c, s1.at[d, r], r1.at[x, r]))
        go(ag_copy(buf, x, r, partner, s2.at[x, r], r2.at[x, r]))

    def ag_forward(buf, r, sems):
        s1, r1, s2, r2 = sems
        for d in range(1, n_x):
            sx = lax.rem(x + d, n_x)
            ag_copy(buf, sx, r, partner, s1.at[d, r], r1.at[sx, r]).wait_recv()
            go(ag_copy(buf, sx, r, partner, s2.at[sx, r], r2.at[sx, r]))

    def ag_finish(buf, r, sems):
        s1, r1, s2, r2 = sems
        for sx in range(n_x):
            ref = buf.at[sx * 2 + (1 - c), rows_of(r), :]
            pltpu.make_async_remote_copy(
                src_ref=ref, dst_ref=ref, send_sem=s2.at[sx, r], recv_sem=r2.at[sx, r],
                device_id=(grp, z, partner), device_id_type=MESH).wait_recv()

    def norm_rows(src, gain, r):
        def body(i, _):
            rows = rows_of(r * (RC // 64) + i, 64)
            total = jnp.zeros((64, 1), F32)
            for b in range(n_t):
                val = src[b, rows, :].astype(F32)
                total = total + jnp.sum(val * val, axis=-1, keepdims=True)
            inv = lax.rsqrt(total / D + EPS)
            for b in range(n_t):
                val = src[b, rows, :].astype(F32)
                xn[rows, b * bw:(b + 1) * bw] = (val * inv * gain[:, b * bw:(b + 1) * bw]).astype(BF)
            return 0
        lax.fori_loop(0, RC // 64, body, 0)

    def product(lhs, rhs, dst, block, r):
        for j in range(per_block):
            dst[block, rows_of(r), j * slotw:(j + 1) * slotw] = jnp.dot(
                lhs[rows_of(r), :], rhs[block * per_block + j], preferred_element_type=F32).astype(BF)

    def rs_copy(src_ref, dst_ref, dest, ssem, rsem):
        return pltpu.make_async_remote_copy(
            src_ref=src_ref, dst_ref=dst_ref, send_sem=ssem, recv_sem=rsem,
            device_id=(grp, z, dest), device_id_type=MESH)

    def reduce(lhs, rhs, prt, r_a, stage, r_b, sems, base, emit):
        s1, r1, s2, r2 = sems

        def to_partner(d, r):
            bx = lax.rem(x + d, n_x)
            return rs_copy(prt.at[bx * 2 + 1 - c, rows_of(r), :], r_a.at[d, rows_of(r), :],
                           partner, s1.at[d, r], r1.at[d, r])

        def across(d, r):
            return rs_copy(stage.at[d, rows_of(r), :], r_b.at[d, rows_of(r), :],
                           lax.rem(x + d, n_x) * 2 + c, s2.at[d, r], r2.at[d, r])

        def combine(d, r):
            bx = lax.rem(x + d, n_x)
            to_partner(d, r).wait_recv()
            stage[d, rows_of(r), :] = (prt[bx * 2 + c, rows_of(r), :].astype(F32)
                                       + r_a[d, rows_of(r), :].astype(F32)).astype(BF)
            go(across(d, r))

        work = [(d, r) for d in range(1, n_x) for r in range(R)]
        prev = None
        for d, r in work + [(0, r) for r in range(R)]:
            bx = lax.rem(x + d, n_x)
            product(lhs, rhs, prt, bx * 2 + 1 - c, r)
            go(to_partner(d, r))
            product(lhs, rhs, prt, bx * 2 + c, r)
            if prev is not None and prev[0] > 0:
                combine(*prev)
            prev = (d, r)
            if r % 2 == 1:
                pump(1)
        for r in range(R):
            pump(1)
            to_partner(0, r).wait_recv()
            total = prt[t, rows_of(r), :].astype(F32) + r_a[0, rows_of(r), :].astype(F32)
            for d in range(1, n_x):
                across(d, r).wait_recv()
                total = total + r_b[d, rows_of(r), :].astype(F32)
            emit(r, (base[t, rows_of(r), :].astype(F32) + total).astype(BF))

    pl.semaphore_wait(barrier, len(friends))
    local[0].wait()
    agx = (a1s, a1r, a2s, a2r)
    for r in range(R):
        ag_start(xw, r, agx)
    for cp in local[1:]:
        cp.wait()
    send_own(2)
    pump(1)
    for r in range(R):
        ag_forward(xw, r, agx)
    pump(1)
    for r in range(R):
        ag_finish(xw, r, agx)
        norm_rows(xw, mg, r)
        pump(1)
    arrive_all("qkvg")
    send_own(5)

    def project(r, _):
        rows = rows_of(r)
        lhs = xn[rows, :]
        for i, dst in enumerate((qr, kr, vr, gr)):
            val = jnp.dot(lhs, wq[:, i * width:(i + 1) * width], preferred_element_type=F32).astype(BF)
            if i >= 2:
                dst[rows, :] = val
                continue
            for h in range(heads):
                part_h = val[:, h * HEAD:(h + 1) * HEAD].astype(F32)
                dst[rows, h * HEAD:(h + 1) * HEAD] = (
                    part_h * cos_ref[rows, :] + pltpu.roll(part_h, HEAD // 2, 1) * sin_ref[rows, :]).astype(BF)
        return 0

    for r in range(R):
        project(r, 0)
        pump(1)
    for h in range(heads):
        cols = slice(h * HEAD, (h + 1) * HEAD)
        for r in range(R):
            span = (r + 1) * RC
            qh = qr[r * RC:(r + 1) * RC, cols]
            scores = lax.dot_general(qh, kr[0:span, cols], (((1,), (1,)), ((), ())),
                                     preferred_element_type=F32)
            gap = (r * RC + lax.broadcasted_iota(jnp.int32, (RC, span), 0)
                   - lax.broadcasted_iota(jnp.int32, (RC, span), 1))
            causal = gap >= 0
            rate = ld_ref[h:h + 1, 0:1]
            fade = jnp.where(causal, jnp.exp(rate * jnp.where(causal, gap, 0).astype(F32)), 0.0)
            weights = (scores * HEAD ** (-0.5) * fade).astype(BF)
            kept = jnp.dot(weights, vr[0:span, cols], preferred_element_type=F32)
            kept = kept * lax.rsqrt(jnp.mean(kept * kept, axis=-1, keepdims=True) + EPS)
            gate = gr[r * RC:(r + 1) * RC, cols].astype(F32)
            ho[r * RC:(r + 1) * RC, cols] = (kept * hg[:, cols] * (gate / (1.0 + jnp.exp(-gate)))).astype(BF)
            if r != 1:
                pump(1)
    arrive_all("out")
    agm = (c1s, c1r, c2s, c2r)

    def emit_mixed(r, val):
        mw[t, rows_of(r), :] = val
        ag_start(mw, r, agm)

    reduce(ho, ob, part, ra, st, rb, (b1s, b1r, b2s, b2r), xw, emit_mixed)
    for r in range(R):
        ag_forward(mw, r, agm)
        if r % 2 == 0:
            pump(1)
    for r in range(R):
        ag_finish(mw, r, agm)
        norm_rows(mw, cg, r)
        pump(1)
    arrive_all("up")

    lift[0:16, :] = jnp.zeros((16, F), BF)
    swit[0:16, :] = jnp.zeros((16, F), BF)

    def widen(weights, dst, r):
        dst[pl.ds(16 + r * RC, RC), :] = jnp.dot(
            xn[rows_of(r), :], weights[...], preferred_element_type=F32).astype(BF)

    for r in range(R):
        widen(ub, lift, r)
        pump(1)
    arrive_all("switch")
    edges = list(range(0, F, 256)) + [F]

    def conv_rows(i, _):
        for lo, hi in zip(edges[:-1], edges[1:]):
            mixed = []
            for src, taps in ((lift, fu), (swit, fsw)):
                val = src[pl.ds(pl.multiple_of(i * 64, 64), 80), lo:hi].astype(F32)
                acc = pltpu.roll(val, 2, 0)[16:] * taps[0:1, lo:hi]
                acc = acc + pltpu.roll(val, 1, 0)[16:] * taps[1:2, lo:hi]
                mixed.append(acc + val[16:] * taps[2:3, lo:hi])
            a, b = mixed
            hid[rows_of(i, 64), lo:hi] = (a * (b / (1.0 + jnp.exp(-b)))).astype(BF)
        return 0

    for r in range(R):
        widen(sb, swit, r)
        pump(1)
        for part_r in range(2):
            first = r * (RC // 64) + part_r * (RC // 128)
            lax.fori_loop(first, first + RC // 128, conv_rows, 0)
            pump(1)

    def emit_out(r, val):
        o_ref[rows_of(r), :] = val

    def slot_reduce(s, way):
        slot = z - s if way == 0 else z + s
        here = (slot >= 0) if way == 0 else (slot < n_f)
        b = jnp.clip(slot, 0, n_f - 1)
        bx, bc = b // 2, b % 2
        d = lax.rem(bx - x + n_x, n_x)
        to_other = jnp.logical_and(here, bc != c)
        relay = jnp.logical_and(jnp.logical_and(here, bc == c), bx != x)
        if s > 0:
            @pl.when(here)
            def _():
                for p in downs:
                    arrive_from(p, b)
        ups, outs = [], []
        for r in range(R):
            up = rs2(part2.at[b, rows_of(r), :], ra2.at[d, rows_of(r), :], partner, d1s.at[d, r], d1r.at[d, r])
            out = rs2(st2.at[d, rows_of(r), :], rb2.at[d, rows_of(r), :], bx * 2 + c, d2s.at[d, r], d2r.at[d, r])
            pending.append((to_other, up))
            pending.append((relay, out))
            ups.append(up)
            outs.append(out)

        for r in range(R):
            @pl.when(here)
            def _(r=r):
                product(hid, db, part2, b, r)

            @pl.when(to_other)
            def _(r=r):
                ups[r].start()

        def second():
            for r in range(R):
                @pl.when(relay)
                def _(r=r):
                    ups[r].wait_recv()
                    st2[d, rows_of(r), :] = (part2[b, rows_of(r), :].astype(F32)
                                             + ra2[d, rows_of(r), :].astype(F32)).astype(BF)
                    outs[r].start()
        return second

    rs2 = rs_copy
    if by_source:
        slot_reduce(0, 0)()
        for s in range(1, n_f):
            while state["ev"] < len(order) and order[state["ev"]][1] <= s:
                pump()
            later = [slot_reduce(s, way) for way in (0, 1)]
            for act in later:
                act()
        for r in range(R):
            rs2(part2.at[t, rows_of(r), :], ra2.at[0, rows_of(r), :], partner, d1s.at[0, r], d1r.at[0, r]).wait_recv()
            total = part2[t, rows_of(r), :].astype(F32) + ra2[0, rows_of(r), :].astype(F32)
            for d in range(1, n_x):
                rs2(st2.at[d, rows_of(r), :], rb2.at[d, rows_of(r), :], lax.rem(x + d, n_x) * 2 + c,
                    d2s.at[d, r], d2r.at[d, r]).wait_recv()
                total = total + rb2[d, rows_of(r), :].astype(F32)
            emit_out(r, (mw[t, rows_of(r), :].astype(F32) + total).astype(BF))
    else:
        arrive_all("down")
        reduce(hid, db, part2, ra2, st2, rb2, (d1s, d1r, d2s, d2r), mw, emit_out)

    for cond, cp in pending:
        if cond is None:
            cp.wait_send()
        else:
            @pl.when(cond)
            def _(cp=cp):
                cp.wait_send()


def on_device(cfg, inputs, mixer_gain, query_weight, key_weight, value_weight, gate_weight, head_gain,
              out_weight, channel_gain, up_weight, switch_weight, filter_up, filter_switch, down_weight):
    n_g, n_f, n_t = cfg
    n_x = n_t // 2
    T, bw = inputs.shape
    D = bw * n_t
    fr, width = query_weight.shape
    heads = width // HEAD
    F = up_weight.shape[1]
    slotw = out_weight.shape[1]
    half = HEAD // 2
    frequency = 10000.0 ** (-jnp.arange(half, dtype=F32) * 2.0 / HEAD)
    angles = jnp.arange(T, dtype=jnp.int32).astype(F32)[:, None] * frequency[None, :]
    cosine, sine = jnp.cos(angles), jnp.sin(angles)
    cos2 = jnp.concatenate([cosine, cosine], axis=1)
    sin2 = jnp.concatenate([-sine, sine], axis=1)
    ids = (lax.axis_index("tp") * heads + jnp.arange(heads, dtype=jnp.int32)).astype(F32)
    rate = jnp.broadcast_to(jnp.log1p(-jnp.exp2(-5.0 - ids))[:, None], (heads, 128))

    n_p = (chunks_of(fr // n_g) * 3 + 1 + chunks_of(down_weight.shape[0] // n_g, 4))
    R = T // 256
    dma = pltpu.SemaphoreType.DMA
    anyspec = pl.BlockSpec(memory_space=pl.ANY)
    vspec = pl.BlockSpec(memory_space=pltpu.VMEM)
    tp_sems = [dma((n_x, R))] * 16
    act = pltpu.VMEM((n_t, T, bw), BF)
    xblk = pltpu.VMEM((n_x, T, bw), BF)
    scratch = [
        pltpu.VMEM((D, 4 * width), BF),
        pltpu.VMEM((n_f,) + out_weight.shape, BF),
        pltpu.VMEM((D, F), BF),
        pltpu.VMEM((D, F), BF),
        pltpu.VMEM((n_f,) + down_weight.shape, BF),
        act,
        pltpu.VMEM((T, D), BF),
        pltpu.VMEM((T, width), BF), pltpu.VMEM((T, width), BF),
        pltpu.VMEM((T, width), BF), pltpu.VMEM((T, width), BF),
        pltpu.VMEM((T, width), BF),
        act, xblk, xblk, xblk,
        act,
        pltpu.VMEM((T + 16, F), BF), pltpu.VMEM((T + 16, F), BF), pltpu.VMEM((T, F), BF),
        act, xblk, xblk, xblk,
        dma((9,)),
        dma((n_p, 2 * n_f)), dma((n_p, n_f)), dma((n_p, n_f * n_g)), dma((n_p, n_f * n_g)),
    ] + tp_sems
    flops = 2 * T * (D * 4 * width + width * D + 3 * D * F)
    call = pl.pallas_call(
        functools.partial(kernel, cfg),
        out_shape=jax.ShapeDtypeStruct((T, bw), BF),
        in_specs=[anyspec, vspec, anyspec, anyspec, anyspec, anyspec, vspec, anyspec, vspec, anyspec, anyspec,
                  vspec, vspec, anyspec, vspec, vspec, vspec],
        out_specs=vspec,
        scratch_shapes=scratch,
        compiler_params=pltpu.CompilerParams(
            collective_id=0, has_side_effects=True, vmem_limit_bytes=67043328),
        cost_estimate=pl.CostEstimate(flops=flops, bytes_accessed=2 * (D * F * 3), transcendentals=0),
    )
    return call(inputs, mixer_gain[None, :], query_weight, key_weight, value_weight, gate_weight,
                head_gain[None, :], out_weight, channel_gain[None, :], up_weight, switch_weight,
                filter_up, filter_switch, down_weight, cos2, sin2, rate)


def solution(mesh):
    cfg = (mesh.shape["grp"], mesh.shape["fs"], mesh.shape["tp"])
    return jax.shard_map(
        functools.partial(on_device, cfg),
        mesh=mesh,
        in_specs=(
            P(("grp", "fs"), "tp"),
            P(),
            P("fs", "tp"),
            P("fs", "tp"),
            P("fs", "tp"),
            P("fs", "tp"),
            P("tp"),
            P("tp", "fs"),
            P(),
            P("fs", "tp"),
            P("fs", "tp"),
            P(None, "tp"),
            P(None, "tp"),
            P("tp", "fs"),
        ),
        out_specs=P(("grp", "fs"), "tp"),
        check_vma=False,
    )
```
